32 devices in a mesh: sp: 32 (over z, y, x, core), tp: 1.
Axes of the slice: x: 2, y: 2, z: 4, core: 2. Of those that a mesh axis runs over, the one named last changes fastest.
Arguments:
- queries: bfloat16 [8192, 1024], P('sp', 'tp'), may hold values from -30 to 30
- keys: bfloat16 [8192, 256], P('sp', 'tp'), may hold values from -30 to 30
- values: bfloat16 [8192, 256], P('sp', 'tp'), may hold values from -20 to 20
- gate_totals: float32 [8192, 16], P('sp', 'tp'), may hold values from -8192 to 0, as said below
- documents: int32 [8192], P('sp'), may hold values from 0 to 1, never falling along the last dimension, each value on 1 to 6144 neighbouring positions
- stream: bfloat16 [8192, 2048], P(('sp', 'tp')), may hold values from -3 to 3
- out_weight: bfloat16 [1024, 2048], replicated, may hold values from -0.1875 to 0.1875
- norm_gain: float32 [2048], replicated, may hold values from 0.1 to 1.9
- routes: int32 [8192, 2], P(('sp', 'tp')), may hold values from 0 to 31, all different within a row; in each aligned block of 256 rows (0 to 255, 256 to 511, ...) at most 32 rows name the same one
- route_weights: float32 [8192, 2], P(('sp', 'tp')), may hold values from 0.2 to 1
- expert_gate: bfloat16 [32, 2048, 1024], P('sp', None, 'tp'), may hold values from -0.125 to 0.125
- expert_up: bfloat16 [32, 2048, 1024], P('sp', None, 'tp'), may hold values from -0.125 to 0.125
- expert_down: bfloat16 [32, 1024, 2048], P('sp', 'tp'), may hold values from -0.1875 to 0.1875
Outputs:
- output: bfloat16 [8192, 2048], P(('sp', 'tp'))
The draws below stay inside these ranges and needn't reach their ends.
Inputs may be any that keep to these rules, and one draw needn't show every extreme that they name: `gate_totals`: along positions it never rises, for every head. `routes`: in each aligned block of rows held by one device, no expert is named by more than 32 rows.
All inputs are finite; a program needn't handle non-finite values.
Results may differ from the reference program's by a relative error of at most 0.014.
Values may be sent and summed in bfloat16 or wider, within the bound.
No kernel may reach another device: no remote copies, remote signals or barrier semaphores. Data moves between devices by JAX's collectives and lax.ppermute only.
A program may use at most 128 MiB of HBM per device.

```python
import math
import jax
import jax.numpy as jnp
import numpy as np
from jax import lax

D = 2048
QUERY_HEAD_COUNT = 16
KV_HEADS = 4
HD = 64
FF = 1024
TOP = 2
DOCS = 2
TOK_DEV = 256
SEQUENCE_TOKENS = 8192
EXPERTS = 32
CAP = 32
DOC_MOST = 6144
N_SP = 32
N_TP = 1


def draw_keys(key, part):
    base = jax.random.normal(jax.random.fold_in(key, 2), (SEQUENCE_TOKENS, KV_HEADS, HD), jnp.float32)
    return base.reshape(SEQUENCE_TOKENS, KV_HEADS * HD).astype(jnp.bfloat16)


def draw_queries(key, part):
    group = QUERY_HEAD_COUNT // KV_HEADS
    base = jax.random.normal(jax.random.fold_in(key, 1), (SEQUENCE_TOKENS, KV_HEADS, group, HD), jnp.float32)
    return base.reshape(SEQUENCE_TOKENS, QUERY_HEAD_COUNT * HD).astype(jnp.bfloat16)


def draw_gate_totals(key, part):
    ranking = jax.random.permutation(jax.random.fold_in(key, 21), QUERY_HEAD_COUNT)
    faster_variant = ranking < QUERY_HEAD_COUNT // 2
    slow_total = jax.random.uniform(jax.random.fold_in(key, 22), (QUERY_HEAD_COUNT,), jnp.float32, 0.15, 0.5)
    quick_rate = 1.0 / jax.random.uniform(jax.random.fold_in(key, 23), (QUERY_HEAD_COUNT,), jnp.float32, 30.0, 60.0)
    decay_speed = jnp.where(faster_variant, quick_rate, slow_total / SEQUENCE_TOKENS)
    machine_multiplier = jnp.exp(jax.random.uniform(jax.random.fold_in(key, 24), (SEQUENCE_TOKENS // TOK_DEV, 1), jnp.float32, -0.7, 0.7))
    machine_multiplier = jnp.repeat(machine_multiplier, TOK_DEV, axis=0)
    coarse_estimate = jax.random.uniform(jax.random.fold_in(key, 25), (SEQUENCE_TOKENS, QUERY_HEAD_COUNT), jnp.float32, 0.4, 1.6)
    cluster_positions = jax.random.randint(jax.random.fold_in(key, 26), (2, QUERY_HEAD_COUNT), 0, SEQUENCE_TOKENS)
    cluster_dropout = jnp.log(jax.random.uniform(jax.random.fold_in(key, 27), (2, QUERY_HEAD_COUNT), jnp.float32, 0.55, 0.8))
    locations = jnp.arange(SEQUENCE_TOKENS, dtype=jnp.int32)[:, None]
    token_clusters = jnp.where(locations == cluster_positions[0][None, :], cluster_dropout[0][None, :], 0.0)
    token_clusters = token_clusters + jnp.where(locations == cluster_positions[1][None, :], cluster_dropout[1][None, :], 0.0)
    logarithm_gate = -decay_speed[None, :] * machine_multiplier * coarse_estimate + jnp.where(faster_variant[None, :], 0.0, token_clusters)
    return jnp.cumsum(logarithm_gate, axis=0).astype(jnp.float32)


def shard_levels(rng, shape, shards, smallest, top_value):
    loudness = 1.0
    for axis_at, parts in shards:
        heights = jax.random.uniform(jax.random.fold_in(jax.random.fold_in(rng, 6), axis_at), (parts,), jnp.float32, smallest / len(shards), top_value / len(shards))
        loudness = loudness * jnp.repeat(jnp.exp(heights), shape[axis_at] // parts).reshape((-1,) + (1,) * (len(shape) - 1 - axis_at))
    return loudness


def length_profile(count, total, bound, slope):
    loads = [(1 << 20) // math.isqrt(grade ** slope) + 1 for grade in range(2, count + 1)]
    rest, counts = total - bound - (count - 1), [1] * (count - 1)
    while rest > 0:
        free = [i for i in range(count - 1) if counts[i] < bound]
        whole, remaining = sum([loads[i] for i in free]), rest
        for i in free:
            extra = min(bound - counts[i], max(1, remaining * loads[i] // whole), rest)
            counts[i] = counts[i] + extra
            rest = rest - extra
    return np.array([bound] + counts)


def ragged_sizes(stream_key, amount, total, most, slope):
    if amount == 2:
        one = jax.random.randint(stream_key, (), max(1, total - most), min(most, total - 1) + 1)
        return jnp.stack([one, total - one])
    tallies = jnp.asarray(length_profile(amount, total, most, slope), jnp.int32)
    twos = (amount - 1) // 2
    donor, receiver = tallies[1:1 + 2 * twos:2], tallies[2:2 + 2 * twos:2]
    slack = jnp.minimum(donor - 1, most - receiver)
    shifted = jax.random.randint(jax.random.fold_in(stream_key, 1), (twos,), 0, 1 << 20) % (slack + 1)
    tallies = tallies.at[1:1 + 2 * twos:2].set(donor - shifted).at[2:2 + 2 * twos:2].set(receiver + shifted)
    return tallies[jax.random.permutation(jax.random.fold_in(stream_key, 2), amount)]


def assign_block(own_key, own, number, rows, amount, top, most, slope):
    order = jax.random.permutation(own_key, amount)
    crowded, usual = portions_of(amount, rows * top, most, slope, True), portions_of(amount, rows * top, most, slope, False)
    places = jnp.arange(amount)

    def named(sizes, offset_by):
        used = int((sizes > 0).sum())
        fixed = max(1, used // 4)
        passed = fixed + (places - fixed + offset_by * (used - fixed)) % max(1, amount - fixed)
        return jnp.zeros((amount,), jnp.int32).at[order[jnp.where(places < fixed, places, passed)]].set(jnp.asarray(sizes, jnp.int32))

    sizes = jnp.where(number % 4 == 0, named(crowded, number // 4), named(usual, number - number // 4 - 1))
    mixed = jax.random.permutation(jax.random.fold_in(own, 3), amount)
    donor, taker = mixed[0:amount // 2 * 2:2], mixed[1:amount // 2 * 2:2]
    slack = jnp.minimum(sizes[donor] - 1, most - sizes[taker]) // 2
    slack = jnp.where((donor == order[0]) | (taker == order[0]) | (sizes[taker] == 0), 0, jnp.maximum(slack, 0))
    passed = jax.random.randint(jax.random.fold_in(own, 4), (amount // 2,), 0, 1 << 20) % (slack + 1)
    sizes = sizes.at[donor].add(-passed).at[taker].add(passed)
    labels = jnp.searchsorted(jnp.cumsum(sizes), jnp.arange(rows * top), side="right").astype(jnp.int32)
    table = labels.reshape(top, rows).T
    table = table[jax.random.permutation(jax.random.fold_in(own, 1), rows)]
    offset_by = jax.random.randint(jax.random.fold_in(own, 2), (rows, 1), 0, top)
    return jnp.take_along_axis(table, (jnp.arange(top)[None, :] + offset_by) % top, axis=1)


def portions_of(amount, total, bound, slope, full):
    weights = [(1 << 20) // math.isqrt(standing ** slope) + 1 for standing in range(1, amount + 1)]
    largest = bound if full else min(bound, max(-(-total // amount), total * weights[0] // sum(weights)))
    least = 1 if total - largest >= amount - 1 else 0
    counts, spare = [largest] + [least] * (amount - 1), total - largest - least * (amount - 1)
    while spare > 0:
        free = [i for i in range(1, amount) if counts[i] < largest] or [i for i in range(1, amount) if counts[i] < bound]
        whole, budget = sum([weights[i] for i in free]), spare
        for i in free:
            more = min(bound - counts[i], max(1, budget * weights[i] // whole), spare)
            counts[i] = counts[i] + more
            spare = spare - more
    return np.array(counts)


def normal_values(key, extent, deviation, reach, split=(), kind=jnp.bfloat16):
    values = jax.random.normal(key, extent, jnp.float32) * deviation
    if len(split) > 0:
        values = shard_levels(key, extent, split, -0.22, 0.18) * values
    return jnp.clip(values, min=-reach, max=reach).astype(kind)


def setup_inputs(seed: int = 0) -> dict:
    splits = jax.random.split(jax.random.key(seed), 14)
    queries = draw_queries(jax.random.fold_in(splits[13], 71), 0)
    keys = draw_keys(jax.random.fold_in(splits[13], 71), 0)
    values = normal_values(splits[2], (SEQUENCE_TOKENS, KV_HEADS * HD), 4.0, 20.0, ((0, 32),))
    gate_totals = draw_gate_totals(jax.random.fold_in(splits[13], 71), 0)
    documents = jnp.searchsorted(jnp.cumsum(ragged_sizes(splits[4], DOCS, SEQUENCE_TOKENS, DOC_MOST, 1)), jnp.arange(SEQUENCE_TOKENS), side="right").astype(jnp.int32)
    stream = normal_values(splits[5], (SEQUENCE_TOKENS, D), 0.5, 3.0, ((0, 32),))
    out_weight = normal_values(splits[6], (QUERY_HEAD_COUNT * HD, D), (QUERY_HEAD_COUNT * HD) ** -0.5, 0.1875)
    norm_gain = jnp.clip(1.0 + 0.18 * jax.random.normal(splits[7], (D,), jnp.float32), 0.1, 1.9)
    routes_keys = jax.random.split(jax.random.fold_in(splits[8], 1), SEQUENCE_TOKENS // (TOK_DEV // N_TP))
    routes_turns = jax.random.permutation(jax.random.fold_in(splits[8], 3), SEQUENCE_TOKENS // (TOK_DEV // N_TP))
    routes = jax.vmap(lambda own, number: assign_block(jax.random.fold_in(splits[8], 2), own, number, TOK_DEV // N_TP, EXPERTS, TOP, CAP, 1))(routes_keys, routes_turns).reshape((SEQUENCE_TOKENS, TOP))
    route_weights = jnp.clip(0.2 + 0.8 * jax.random.uniform(splits[9], (SEQUENCE_TOKENS, TOP), jnp.float32) ** shard_levels(splits[9], (SEQUENCE_TOKENS, TOP), ((0, 32),), -0.2, 0.2), 0.2, 1.0)
    expert_gate = normal_values(splits[10], (EXPERTS, D, FF), D ** -0.5, 0.125, ((0, 32),))
    expert_up = normal_values(splits[11], (EXPERTS, D, FF), D ** -0.5, 0.125, ((0, 32),))
    expert_down = normal_values(splits[12], (EXPERTS, FF, D), FF ** -0.5, 0.1875, ((0, 32),))
    return {"queries": queries, "keys": keys, "values": values, "gate_totals": gate_totals, "documents": documents, "stream": stream, "out_weight": out_weight, "norm_gain": norm_gain, "routes": routes, "route_weights": route_weights, "expert_gate": expert_gate, "expert_up": expert_up, "expert_down": expert_down}


EPS = 1e-06
MASKED = -1e+30

def attend(queries, keys, values, gate_totals, documents):
    group = QUERY_HEAD_COUNT // KV_HEADS
    block = min(256, SEQUENCE_TOKENS)
    scale = HD ** (-0.5)
    key_all = keys.astype(jnp.float32).reshape(SEQUENCE_TOKENS, KV_HEADS, HD)
    value_all = values.astype(jnp.float32).reshape(SEQUENCE_TOKENS, KV_HEADS, HD)
    key_gate = gate_totals.T.reshape(KV_HEADS, group, 1, SEQUENCE_TOKENS)
    key_pos = jnp.arange(SEQUENCE_TOKENS, dtype=jnp.int32)

    def one_block(index):
        start = (index * block).astype(jnp.int32)
        query_blk = lax.dynamic_slice_in_dim(queries, start, block, 0).astype(jnp.float32).reshape(block, KV_HEADS, group, HD)
        query_gate = lax.dynamic_slice_in_dim(gate_totals, start, block, 0).T.reshape(KV_HEADS, group, block, 1)
        query_doc = lax.dynamic_slice_in_dim(documents, start, block, 0)
        query_pos = start + jnp.arange(block, dtype=jnp.int32)
        scores = jnp.einsum('qkgd,skd->kgqs', query_blk, key_all) * scale + query_gate - key_gate
        allowed = (key_pos[None, :] <= query_pos[:, None]) & (documents[None, :] == query_doc[:, None])
        scores = jnp.where(allowed, scores, MASKED)
        highest = lax.optimization_barrier(jnp.max(scores, axis=-1, keepdims=True))
        weights = jnp.where(allowed, jnp.exp(scores - highest), 0.0)
        totals = lax.optimization_barrier(jnp.sum(weights, axis=-1))
        rounded = lax.optimization_barrier(weights.astype(jnp.bfloat16)).astype(jnp.float32)
        mixed = jnp.einsum('kgqs,skd->kgqd', rounded, value_all) / totals[..., None]
        return jnp.transpose(mixed, (2, 0, 1, 3)).reshape(block, QUERY_HEAD_COUNT * HD).astype(jnp.bfloat16)
    blocks = lax.map(one_block, jnp.arange(SEQUENCE_TOKENS // block, dtype=jnp.int32))
    return blocks.reshape(SEQUENCE_TOKENS, QUERY_HEAD_COUNT * HD)

def run_experts(normed, routes, expert_gate, expert_up, expert_down):
    flat = routes.reshape(-1)
    load = N_SP * N_TP * CAP
    half = FF // N_TP

    def one_expert(expert):
        rank_key = jnp.where(flat == expert, 0, 1).astype(jnp.int32)
        order = jnp.argsort(rank_key, stable=True)[:load].astype(jnp.int32)
        valid = flat[order] == expert
        picked = normed[order // TOP]
        gate = jnp.dot(picked, expert_gate[expert], preferred_element_type=jnp.float32)
        upper = jnp.dot(picked, expert_up[expert], preferred_element_type=jnp.float32)
        inner = (jax.nn.silu(gate) * upper).astype(jnp.bfloat16)
        answer = jnp.zeros((load, D), jnp.float32)
        for portion in range(N_TP):
            piece = jnp.dot(inner[:, portion * half:(portion + 1) * half], expert_down[expert][portion * half:(portion + 1) * half], preferred_element_type=jnp.float32)
            answer = answer + lax.optimization_barrier(piece.astype(jnp.bfloat16)).astype(jnp.float32)
        answer = jnp.where(valid[:, None], answer.astype(jnp.bfloat16).astype(jnp.float32), 0.0)
        return (order, answer)
    orders, answers = lax.map(one_expert, jnp.arange(EXPERTS, dtype=jnp.int32))
    entries = jnp.zeros((flat.shape[0], D), jnp.float32).at[orders.reshape(-1)].add(answers.reshape(-1, D))
    return entries.reshape(SEQUENCE_TOKENS, TOP, D)

def reference(queries, keys, values, gate_totals, documents, stream, out_weight, norm_gain, routes, route_weights, expert_gate, expert_up, expert_down):
    attended = attend(queries, keys, values, gate_totals, documents)
    hidden = (stream.astype(jnp.float32) + jnp.dot(attended, out_weight, preferred_element_type=jnp.float32)).astype(jnp.bfloat16)
    hidden_f = hidden.astype(jnp.float32)
    normed = (hidden_f * lax.rsqrt(lax.optimization_barrier(jnp.mean(hidden_f * hidden_f, axis=-1, keepdims=True)) + EPS) * norm_gain).astype(jnp.bfloat16)
    entries = run_experts(normed, routes, expert_gate, expert_up, expert_down)
    routed = lax.optimization_barrier(jnp.sum(route_weights[..., None] * entries, axis=1))
    return (hidden_f + routed).astype(jnp.bfloat16)
```

```python
import math

import jax
import jax.numpy as jnp
from jax import lax
from jax.experimental import pallas as pl
from jax.experimental.pallas import tpu as pltpu
from jax.sharding import PartitionSpec as P


QUERY_HEAD_COUNT = 16
KV_HEADS = 4
HD = 64
TOP = 2
GROUP = QUERY_HEAD_COUNT // KV_HEADS

EPS = 1e-06
MASKED = -1e30

EXT = 16
DOC_ROW = 3 * GROUP
COUNT_ROW = DOC_ROW + 1
ONES_ROW = DOC_ROW + 2
PACK = 2 * HD + EXT
F32 = jnp.float32
BF16 = jnp.bfloat16

CHUNK = 512
WIDE_CHUNK = 1024


def make_fold(query_rows, query_gate, key_gate_all, query_docs, first_pos, kv_local, group):
    count = query_rows.shape[0]
    scale = HD ** (-0.5)
    query_blk = query_rows.reshape(count, kv_local, group, HD)
    gate_here = query_gate.T.reshape(kv_local, group, count, 1)
    query_pos = first_pos + jnp.arange(count, dtype=jnp.int32)
    last_pos = first_pos + count - 1
    first_doc = query_docs[0]

    def block_step(carry, block_in):
        running_max, running_sum, carried = carry
        key_block, value_block, doc_block, pos_block = block_in
        width = key_block.shape[0]

        def compute(unused):
            key_heads = key_block.reshape(width, kv_local, HD)
            value_heads = value_block.reshape(width, kv_local, HD)
            gate_keys = lax.dynamic_slice_in_dim(key_gate_all, pos_block[0], width, 0).T.reshape(
                kv_local, group, 1, width
            )
            scores = (
                jnp.einsum(
                    "qkgd,nkd->kgqn", query_blk, key_heads, preferred_element_type=jnp.float32
                )
                * scale
                + gate_here
                - gate_keys
            )
            allowed = (pos_block[None, :] <= query_pos[:, None]) & (
                doc_block[None, :] == query_docs[:, None]
            )
            scores = jnp.where(allowed, scores, MASKED)
            new_max = jnp.maximum(running_max, jnp.max(scores, axis=-1))
            weights = jnp.where(allowed, jnp.exp(scores - new_max[..., None]), 0.0)
            factor = jnp.exp(running_max - new_max)
            new_sum = running_sum * factor + jnp.sum(weights, axis=-1)
            new_carried = carried * factor[..., None] + jnp.einsum(
                "kgqn,nkd->kgqd",
                weights.astype(jnp.bfloat16),
                value_heads,
                preferred_element_type=jnp.float32,
            )
            return (new_max, new_sum, new_carried)

        skipped = (pos_block[0] > last_pos) | (doc_block[width - 1] < first_doc)
        return (lax.cond(skipped, lambda unused: carry, compute, 0), None)

    def fold(carry, piece, start):
        key_piece, value_piece, doc_piece = piece
        length = key_piece.shape[0]
        width = math.gcd(length, 512)
        blocks_count = length // width
        pos_piece = jnp.arange(length, dtype=jnp.int32)
        blocks = (
            key_piece.reshape(blocks_count, width, -1),
            value_piece.reshape(blocks_count, width, -1),
            doc_piece.reshape(blocks_count, width),
            pos_piece.reshape(blocks_count, width),
        )
        carry, _ = lax.scan(block_step, carry, blocks)
        return carry

    initial = (
        jnp.full((kv_local, group, count), MASKED, jnp.float32),
        jnp.zeros((kv_local, group, count), jnp.float32),
        jnp.zeros((kv_local, group, count, HD), jnp.float32),
    )
    return (fold, initial)


def finish(running_sum, carried):
    mixed = carried / running_sum[..., None]
    count = mixed.shape[2]
    return jnp.transpose(mixed, (2, 0, 1, 3)).reshape(count, -1).astype(jnp.bfloat16)


def shards(
    queries,
    keys,
    values,
    gate_totals,
    documents,
    stream,
    out_weight,
    norm_gain,
    routes,
    route_weights,
    expert_gate,
    expert_up,
    expert_down,
):
    tp_count = lax.axis_size("tp")
    tp_index = lax.axis_index("tp")
    sp_index = lax.axis_index("sp")
    group = QUERY_HEAD_COUNT // KV_HEADS
    tok_local = queries.shape[0]
    own_rows = tok_local // tp_count
    first_row = sp_index * tok_local
    query_rows = lax.all_to_all(queries, "tp", split_axis=0, concat_axis=1, tiled=True)
    key_whole, value_whole = (
        lax.all_gather(keys, "tp", axis=1, tiled=True),
        lax.all_gather(values, "tp", axis=1, tiled=True),
    )
    gate_whole = lax.all_gather(gate_totals, "tp", axis=1, tiled=True)
    key_gate_all = lax.all_gather(gate_whole, "sp", axis=0, tiled=True)
    query_gate = lax.dynamic_slice_in_dim(gate_whole, tp_index * own_rows, own_rows, 0)
    query_docs = lax.dynamic_slice_in_dim(documents, tp_index * own_rows, own_rows, 0)
    fold, initial = make_fold(
        query_rows,
        query_gate,
        key_gate_all,
        query_docs,
        first_row + tp_index * own_rows,
        KV_HEADS,
        group,
    )
    _, running_sum, carried = fold(
        initial,
        (
            lax.all_gather(key_whole, "sp", axis=0, tiled=True),
            lax.all_gather(value_whole, "sp", axis=0, tiled=True),
            lax.all_gather(documents, "sp", axis=0, tiled=True),
        ),
        jnp.int32(0),
    )
    attended = finish(running_sum, carried)
    hidden = (
        stream.astype(jnp.float32)
        + jnp.dot(attended, out_weight, preferred_element_type=jnp.float32)
    ).astype(jnp.bfloat16)
    hidden_f = hidden.astype(jnp.float32)
    normed = (
        hidden_f
        * lax.rsqrt(jnp.mean(hidden_f * hidden_f, axis=-1, keepdims=True) + EPS)
        * norm_gain
    ).astype(jnp.bfloat16)
    return experts_direct(
        hidden, normed, routes, route_weights, expert_gate, expert_up, expert_down
    )


def experts_direct(hidden, normed, routes, route_weights, expert_gate, expert_up, expert_down):
    tp_count = lax.axis_size("tp")
    sp_count = lax.axis_size("sp")
    hidden_f = hidden.astype(jnp.float32)
    own_rows = hidden.shape[0]
    tok_local = own_rows * tp_count
    local_experts = expert_gate.shape[0]
    experts_total = local_experts * sp_count
    capacity = max(2, 2 * tok_local * TOP // (tp_count * experts_total))
    flat = routes.reshape(-1)
    hits = (flat[:, None] == jnp.arange(experts_total, dtype=jnp.int32)[None, :]).astype(jnp.int32)
    slot_index = jnp.sum(jnp.cumsum(hits, axis=0) * hits, axis=1) - 1
    target = flat * capacity + slot_index
    entry_rows = jnp.repeat(normed, TOP, axis=0)
    outgoing = (
        jnp.zeros((experts_total * capacity, normed.shape[1]), jnp.bfloat16)
        .at[target]
        .set(entry_rows)
    )
    outgoing = outgoing.reshape(experts_total, capacity, -1)
    arrived = lax.all_to_all(outgoing, "sp", split_axis=0, concat_axis=0, tiled=True)
    slots = arrived.shape[1]
    both_halves = lax.all_gather(arrived, "tp", axis=0, tiled=True)
    grouped = both_halves.reshape(tp_count * sp_count, local_experts, slots, -1)
    gate = jnp.einsum("secd,edf->secf", grouped, expert_gate, preferred_element_type=jnp.float32)
    upper = jnp.einsum("secd,edf->secf", grouped, expert_up, preferred_element_type=jnp.float32)
    inner = (jax.nn.silu(gate) * upper).astype(jnp.bfloat16)
    partial_value = jnp.einsum(
        "secf,efd->secd", inner, expert_down, preferred_element_type=jnp.float32
    )
    partial_value = lax.optimization_barrier(partial_value.astype(jnp.bfloat16)).astype(jnp.float32)
    summed = lax.psum_scatter(
        partial_value.reshape(tp_count * sp_count * local_experts, slots, -1).astype(jnp.bfloat16),
        "tp",
        scatter_dimension=0,
        tiled=True,
    )
    returned = lax.all_to_all(summed, "sp", split_axis=0, concat_axis=0, tiled=True)
    answers = returned.reshape(experts_total * capacity, -1)[target].reshape(own_rows, TOP, -1)
    routed = jnp.sum(route_weights[..., None] * answers.astype(jnp.float32), axis=1)
    return (hidden_f + routed).astype(jnp.bfloat16)


def xor_permute(x, distance, count):
    return lax.ppermute(x, "sp", [(s, s ^ distance) for s in range(count)])


def attention_kernel(per, planes, blk, dists, *refs):
    nq = len(dists)
    ids_ref = refs[0]
    q_refs = refs[1 : 1 + nq]
    kv_refs = refs[1 + nq : 1 + nq + per]
    o_refs = refs[1 + nq + per : 1 + 2 * nq + per]
    most_ref = refs[1 + 2 * nq + per]
    kvs, qa, m_ref, acc_ref, o_all, sems = refs[2 + 2 * nq + per :]
    copies = [
        pltpu.make_async_copy(kv_refs[k], kvs.at[pl.ds(k * planes, planes)], sems.at[k])
        for k in range(per)
    ]
    for c in copies:
        c.start()
    plane, place = ids_ref[0], ids_ref[1]
    lane = lax.broadcasted_iota(jnp.int32, (blk, EXT), 1)
    for i in range(nq):
        for h in range(GROUP):
            qa[i * GROUP + h, :, 0:HD] = q_refs[i][:, h * HD : (h + 1) * HD] * jnp.asarray(
                HD ** (-0.5), BF16
            )
            pick = (lane == h) | (lane == GROUP + h) | (lane == 2 * GROUP + h)
            qa[i * GROUP + h, :, HD : HD + EXT] = jnp.where(pick, -1.0, 0.0).astype(BF16)
    for c in copies:
        c.wait()
    ext_sum = jnp.zeros((EXT, blk), F32)
    ext_max = jnp.zeros((EXT, blk), F32)
    for b in range(per * planes):
        ext = kvs[b, HD : HD + EXT, :].astype(F32)
        ext_sum = ext_sum + ext
        ext_max = jnp.maximum(ext_max, ext)
    row = lax.broadcasted_iota(jnp.int32, (EXT, blk), 0)
    later = jnp.sum(jnp.where(row == DOC_ROW, ext_sum, 0.0)).astype(jnp.int32)
    border = per * planes * blk - later
    most_ref[0] = jnp.max(jnp.where(row == COUNT_ROW, ext_max, 0.0)).astype(jnp.int32)

    def one_block(i, unused):
        dist = jnp.int32(dists[0])
        for n in range(1, nq):
            dist = jnp.where(i == n, dists[n], dist)
        block = (plane ^ dist) * per + place
        first = block * blk
        begin = jnp.where(first >= border, border, 0)
        last_begin = jnp.where(first + blk > border, border, 0)
        low = begin // blk
        free = jnp.minimum(block, (last_begin + blk - 1) // blk)
        free = free + lax.rem(block - free, 2)
        for h in range(GROUP):
            m_ref[h] = jnp.full((blk, 128), MASKED, F32)
            acc_ref[h] = jnp.zeros((blk, EXT + HD), F32)

        def where_is(kb):
            return ((kb % per) ^ place) * planes + ((kb // per) ^ plane)

        def step(kbs, masked):
            at = [where_is(kb) for kb in kbs]
            if masked:
                pos_q = first + lax.broadcasted_iota(jnp.int32, (blk, blk), 0)
                pos_k = kbs[0] * blk + lax.broadcasted_iota(jnp.int32, (blk, blk), 1)
                start_q = jnp.where(pos_q >= border, border, 0)
                allowed = (pos_k <= pos_q) & (pos_k >= start_q)
            for h in range(GROUP):
                scores = [
                    jnp.dot(
                        qa[i * GROUP + h], kvs[a, 0 : HD + EXT, :], preferred_element_type=F32
                    )
                    for a in at
                ]
                if masked:
                    scores = [jnp.where(allowed, s, MASKED) for s in scores]
                old = m_ref[h]
                top = scores[0]
                for s in scores[1:]:
                    top = jnp.maximum(top, s)
                new = jnp.maximum(old, jnp.max(top, axis=1, keepdims=True))
                wide = jnp.concatenate([new] * (blk // 128), axis=1)
                mixed = acc_ref[h] * jnp.exp(old - new)[:, 0 : EXT + HD]
                for s, a in zip(scores, at):
                    weights = jnp.exp(s - wide)
                    if masked:
                        weights = jnp.where(allowed, weights, 0.0)
                    mixed = mixed + lax.dot_general(
                        weights.astype(BF16),
                        kvs[a, HD:PACK, :],
                        (((1,), (1,)), ((), ())),
                        preferred_element_type=F32,
                    )
                m_ref[h] = new
                acc_ref[h] = mixed

        count = free - low + 1

        def masked_step(n, unused):
            step([jnp.where(n == count - 1, block, low + n)], True)
            return 0

        def free_step(n, unused):
            step([free + 2 * n, free + 2 * n + 1], False)
            return 0

        lax.fori_loop(0, (block - free) // 2, free_step, 0)
        lax.fori_loop(0, count, masked_step, 0)
        for h in range(GROUP):
            mixed = acc_ref[h]
            o_all[i, :, h * HD : (h + 1) * HD] = (
                mixed[:, EXT : EXT + HD] / mixed[:, ONES_ROW : ONES_ROW + 1]
            ).astype(BF16)
        return 0

    lax.fori_loop(0, nq, one_block, 0)
    for i in range(nq):
        o_refs[i][...] = o_all[i]


def run_attention(ids, q_blocks, packs, dists, per, planes):
    blk = q_blocks[0].shape[0]
    nq = len(dists)
    vm = pl.BlockSpec(memory_space=pltpu.VMEM)
    sm = pl.BlockSpec(memory_space=pltpu.SMEM)
    hb = pl.BlockSpec(memory_space=pl.ANY)
    pairs = nq * GROUP * blk * per * planes * blk
    out = pl.pallas_call(
        lambda *refs: attention_kernel(per, planes, blk, dists, *refs),
        out_shape=[jax.ShapeDtypeStruct((blk, GROUP * HD), BF16)] * nq
        + [jax.ShapeDtypeStruct((1,), jnp.int32)],
        in_specs=[sm] + [vm] * nq + [hb] * per,
        out_specs=[vm] * nq + [sm],
        scratch_shapes=[
            pltpu.VMEM((per * planes, PACK, blk), BF16),
            pltpu.VMEM((nq * GROUP, blk, HD + EXT), BF16),
            pltpu.VMEM((GROUP, blk, 128), F32),
            pltpu.VMEM((GROUP, blk, EXT + HD), F32),
            pltpu.VMEM((nq, blk, GROUP * HD), BF16),
            pltpu.SemaphoreType.DMA((per,)),
        ],
        compiler_params=pltpu.CompilerParams(vmem_limit_bytes=48 * 1024 * 1024),
        cost_estimate=pl.CostEstimate(
            flops=pairs * 300, transcendentals=pairs, bytes_accessed=4 << 20
        ),
        name="attention",
    )(ids, *q_blocks, *packs)
    return out[:nq], out[nq]


def vmem_spec():
    return pl.BlockSpec(memory_space=pltpu.VMEM)


def prepare_kernel(planes, *refs):
    ids_ref, key_ref, value_ref, gate_ref, doc_ref, route_ref, query_ref = refs[:7]
    pack_refs, q_refs, packed = refs[7 : 7 + planes], refs[7 + planes : 7 + 2 * planes], refs[-1]
    plane, per = ids_ref[0], ids_ref[2]
    heads, blk = gate_ref.shape
    rest = gate_ref[...]
    pieces = []
    for _ in range(3):
        piece = rest.astype(BF16)
        pieces.append(piece)
        rest = rest - piece.astype(F32)
    goes = route_ref[...] // per
    most = jnp.zeros((1, 1), F32)
    for p in range(planes):
        there = jnp.max((goes == p).astype(F32), axis=0, keepdims=True)
        most = jnp.maximum(most, jnp.sum(there, axis=1, keepdims=True))
    row = lax.broadcasted_iota(jnp.int32, (EXT, blk), 0)
    fixed = jnp.where(row == DOC_ROW, doc_ref[...].astype(F32), 0.0)
    fixed = fixed + jnp.where(row == COUNT_ROW, most, 0.0) + jnp.where(row == ONES_ROW, 1.0, 0.0)
    to = lax.broadcasted_iota(jnp.int32, (EXT, heads), 0)
    source = lax.broadcasted_iota(jnp.int32, (EXT, heads), 1)
    key_turned = key_ref[...].astype(F32).T.astype(BF16)
    value_turned = value_ref[...].astype(F32).T.astype(BF16)
    for g in range(KV_HEADS):
        extra = fixed
        for part, piece in enumerate(pieces):
            at = to - part * GROUP
            pick = (at >= 0) & (at < GROUP) & (source == g * GROUP + at)
            extra = extra + jnp.dot(
                jnp.where(pick, 1.0, 0.0).astype(BF16), piece, preferred_element_type=F32
            )
        packed[g, 0:HD, :] = key_turned[g * HD : (g + 1) * HD]
        packed[g, HD : HD + EXT, :] = extra.astype(BF16)
        packed[g, HD + EXT : PACK, :] = value_turned[g * HD : (g + 1) * HD]
    size = GROUP * HD
    for d in range(planes):
        pack_refs[d][0] = packed[plane ^ d]
        q_refs[d][...] = query_ref[:, pl.ds(pl.multiple_of((plane ^ d) * size, size), size)]


def prepare(ids, keys, values, gates, documents, routes, queries, planes):
    blk = queries.shape[0]
    sm = pl.BlockSpec(memory_space=pltpu.SMEM)
    out = pl.pallas_call(
        lambda *refs: prepare_kernel(planes, *refs),
        out_shape=[jax.ShapeDtypeStruct((1, PACK, blk), BF16)] * planes
        + [jax.ShapeDtypeStruct((blk, GROUP * HD), BF16)] * planes,
        in_specs=[sm] + [vmem_spec()] * 6,
        out_specs=[vmem_spec()] * (2 * planes),
        scratch_shapes=[pltpu.VMEM((KV_HEADS, PACK, blk), BF16)],
        name="prepare",
    )(ids, keys, values, gates.T, documents.reshape(1, blk), routes.T, queries)
    return out[:planes], out[planes:]


def fast_attention(ids, queries, keys, values, gate_totals, documents, routes, per, planes):
    count = per * planes
    own, q_groups = prepare(
        ids, keys, values, gate_totals, documents, routes, queries, planes
    )
    column, q_blocks = [own[0]], [q_groups[0]]
    for d in range(1, planes):
        column.append(xor_permute(own[d], d * per, count))
        q_blocks.append(xor_permute(q_groups[d], d * per, count))
    column = jnp.concatenate(column, axis=0)
    packs = {0: column}
    for k in range(2, per, 2):
        packs[k] = xor_permute(column, k, count)
    for k in range(0, per, 2):
        packs[k + 1] = xor_permute(packs[k], 1, count)
    packs = [packs[k] for k in range(per)]
    outs = [None] * planes
    far = list(range(planes - 1, 0, -1))
    far_out, most_all = run_attention(ids, [q_blocks[d] for d in far], packs, far, per, planes)
    for d, o in zip(far, far_out):
        outs[d] = xor_permute(o, d * per, count)
    near_out, _ = run_attention(ids, [q_blocks[0]], packs, [0], per, planes)
    outs[0] = near_out[0]
    return outs, most_all[0]


def project_kernel(planes, limit, *refs):
    ids_ref, stream_ref, weight_ref, gain_ref = refs[:4]
    o_refs = refs[4 : 4 + planes]
    list_refs = refs[4 + planes : 3 + 2 * planes]
    hidden_ref, normed_ref = refs[3 + 2 * planes : 5 + 2 * planes]
    sent_refs = refs[5 + 2 * planes :]
    plane = ids_ref[0]
    rows = o_refs[0].shape[1]
    blk, width = stream_ref.shape
    attended = [o[...] for o in o_refs]

    def columns(c, squares):
        at = pl.ds(pl.multiple_of(c * WIDE_CHUNK, WIDE_CHUNK), WIDE_CHUNK)
        total = stream_ref[:, at].astype(F32)
        for d in range(planes):
            weight = weight_ref[pl.ds(pl.multiple_of((plane ^ d) * rows, rows), rows), at]
            total = total + jnp.dot(attended[d], weight, preferred_element_type=F32)
        hidden = total.astype(BF16)
        hidden_ref[:, at] = hidden
        hidden_f = hidden.astype(F32)
        return squares + jnp.sum(hidden_f * hidden_f, axis=-1, keepdims=True)

    squares = lax.fori_loop(0, width // WIDE_CHUNK, columns, jnp.zeros((blk, 1), F32))
    scale = lax.rsqrt(squares / width + EPS)

    def send(c, unused):
        at = pl.ds(pl.multiple_of(c * WIDE_CHUNK, WIDE_CHUNK), WIDE_CHUNK)
        normed = (hidden_ref[:, at].astype(F32) * scale * gain_ref[:, at]).astype(BF16)
        normed_ref[:, at] = normed
        for d in range(1, planes):
            sent_refs[d - 1][:, at] = jnp.dot(
                list_refs[d - 1][0:limit, :], normed, preferred_element_type=F32
            ).astype(BF16)
        return 0

    lax.fori_loop(0, width // WIDE_CHUNK, send, 0)


def project(ids, outs, stream, out_weight, norm_gain, lists, limit, planes):
    rows, width = stream.shape
    flops = 2 * rows * width * (out_weight.shape[0] + 3 * limit)
    result = pl.pallas_call(
        lambda *refs: project_kernel(planes, limit, *refs),
        out_shape=[jax.ShapeDtypeStruct((rows, width), BF16)] * 2
        + [jax.ShapeDtypeStruct((limit, width), BF16)] * (planes - 1),
        in_specs=[pl.BlockSpec(memory_space=pltpu.SMEM)] + [vmem_spec()] * (2 + 2 * planes),
        out_specs=[vmem_spec()] * (1 + planes),
        compiler_params=pltpu.CompilerParams(vmem_limit_bytes=40 * 1024 * 1024),
        cost_estimate=pl.CostEstimate(flops=flops, transcendentals=0, bytes_accessed=8 << 20),
        name="project",
    )(ids, stream, out_weight, norm_gain.reshape(1, width), *outs, *lists)
    return result[0], result[1], result[2:]


def exact_dot(a, b):
    return jnp.dot(a, b, preferred_element_type=F32).astype(BF16)


def spread_kernel(pick_ref, rows_ref, *outs):
    pick = pick_ref[:, 0 : rows_ref.shape[0]]
    size = outs[0].shape[0]

    def columns(c, unused):
        at = pl.ds(pl.multiple_of(c * CHUNK, CHUNK), CHUNK)
        slots = jnp.dot(pick, rows_ref[:, at], preferred_element_type=F32).astype(BF16)
        for k, out in enumerate(outs):
            out[:, at] = slots[k * size : (k + 1) * size]
        return 0

    lax.fori_loop(0, rows_ref.shape[1] // CHUNK, columns, 0)


def spread(pick, rows, per):
    slots = pick.shape[0]
    limit, width = rows.shape
    return pl.pallas_call(
        spread_kernel,
        out_shape=[jax.ShapeDtypeStruct((slots // per, width), BF16)] * per,
        in_specs=[vmem_spec()] * 2,
        out_specs=[vmem_spec()] * per,
        cost_estimate=pl.CostEstimate(
            flops=2 * slots * limit * width, transcendentals=0, bytes_accessed=2 << 20
        ),
        name="spread",
    )(pick, rows)


def expert_kernel(per, *refs):
    x_refs = refs[:per]
    gate_ref, up_ref, down_ref = refs[per : per + 3]
    o_refs = refs[per + 3 : 2 * per + 3]
    x_all, acc = refs[2 * per + 3 :]
    step = pl.program_id(0)
    size = x_refs[0].shape[0]

    @pl.when(step == 0)
    def fill():
        for k in range(per):
            x_all[k * size : (k + 1) * size, :] = x_refs[k][...]
        acc[...] = jnp.zeros(acc.shape, F32)

    x = x_all[...]
    gate = jnp.dot(x, gate_ref[...], preferred_element_type=F32)
    upper = jnp.dot(x, up_ref[...], preferred_element_type=F32)
    inner = (gate * jax.nn.sigmoid(gate) * upper).astype(BF16)
    acc[...] = acc[...] + jnp.dot(inner, down_ref[...], preferred_element_type=F32)

    @pl.when(step == pl.num_programs(0) - 1)
    def last():
        for k in range(per):
            o_refs[k][...] = acc[k * size : (k + 1) * size, :].astype(BF16)


def run_expert(xs, expert_gate, expert_up, expert_down):
    per = len(xs)
    size, width = xs[0].shape
    units = expert_gate.shape[1]
    chunk = min(256, units)
    whole = pl.BlockSpec((size, width), lambda f: (0, 0))
    return pl.pallas_call(
        lambda *refs: expert_kernel(per, *refs),
        grid=(units // chunk,),
        out_shape=[jax.ShapeDtypeStruct((size, width), BF16)] * per,
        in_specs=[whole] * per
        + [
            pl.BlockSpec((width, chunk), lambda f: (0, f)),
            pl.BlockSpec((width, chunk), lambda f: (0, f)),
            pl.BlockSpec((chunk, width), lambda f: (f, 0)),
        ],
        out_specs=[whole] * per,
        scratch_shapes=[
            pltpu.VMEM((per * size, width), BF16),
            pltpu.VMEM((per * size, width), F32),
        ],
        compiler_params=pltpu.CompilerParams(
            dimension_semantics=("arbitrary",), vmem_limit_bytes=40 * 1024 * 1024
        ),
        cost_estimate=pl.CostEstimate(
            flops=6 * per * size * width * units,
            transcendentals=per * size * units,
            bytes_accessed=14 << 20,
        ),
        name="expert",
    )(*xs, expert_gate, expert_up, expert_down)


def gather_kernel(limit, *refs):
    mix_ref, out_ref = refs[0], refs[-1]

    def columns(c, unused):
        at = pl.ds(pl.multiple_of(c * CHUNK, CHUNK), CHUNK)
        answers = jnp.concatenate([r[:, at] for r in refs[1:-1]], axis=0)
        slots = answers.shape[0]
        total = jnp.dot(mix_ref[0:limit, 0:slots], answers, preferred_element_type=F32)
        total = total + jnp.dot(mix_ref[0:limit, slots:], answers, preferred_element_type=F32)
        out_ref[:, at] = total.astype(out_ref.dtype)
        return 0

    lax.fori_loop(0, out_ref.shape[1] // CHUNK, columns, 0)


def gather_answers(mix, answers, limit, dtype):
    width = answers[0].shape[1]
    return pl.pallas_call(
        lambda *refs: gather_kernel(limit, *refs),
        out_shape=jax.ShapeDtypeStruct((limit, width), dtype),
        in_specs=[vmem_spec()] * (1 + len(answers)),
        out_specs=vmem_spec(),
        cost_estimate=pl.CostEstimate(
            flops=2 * limit * mix.shape[1] * width, transcendentals=0, bytes_accessed=2 << 20
        ),
        name="gather",
    )(mix, *answers)


def finish_kernel(limit, *refs):
    hidden_ref, local_ref, out_ref = refs[0], refs[1], refs[-1]
    others = (len(refs) - 3) // 2
    total = hidden_ref[...].astype(F32) + local_ref[...]
    for turned, back in zip(refs[2 : 2 + others], refs[2 + others : 2 + 2 * others]):
        total = total + jnp.dot(
            turned[:, 0:limit], back[...], preferred_element_type=F32
        )
    out_ref[...] = total.astype(BF16)


def finish_rows(hidden, local, turned, backs):
    rows, width = hidden.shape
    limit = backs[0].shape[0]
    chunk = min(512, width)
    columns = lambda size: pl.BlockSpec((size, chunk), lambda f: (0, f))
    return pl.pallas_call(
        lambda *refs: finish_kernel(limit, *refs),
        grid=(width // chunk,),
        out_shape=jax.ShapeDtypeStruct((rows, width), BF16),
        in_specs=[columns(rows)] * 2
        + [pl.BlockSpec((rows, rows), lambda f: (0, 0))] * len(turned)
        + [columns(limit)] * len(backs),
        out_specs=columns(rows),
        compiler_params=pltpu.CompilerParams(dimension_semantics=("arbitrary",)),
        name="finish",
    )(hidden, local, *turned, *backs)


def route_tables(infos, plane, place, per, planes, capacity):
    rows = infos[0].shape[1]
    routes = jnp.stack([info[:TOP] for info in infos]).astype(jnp.int32)
    weights = jnp.stack([info[TOP:] for info in infos])
    spots = jnp.arange(per, dtype=jnp.int32)
    ids = plane * per + jnp.stack([spots if d in WHOLE else place ^ spots for d in range(planes)])
    hits = routes[:, :, None, :] == ids[:, None, :, None]
    marks = jnp.any(hits, axis=1)
    inside = jnp.any(marks, axis=1)
    bases = (plane ^ jnp.arange(planes, dtype=jnp.int32)) * per
    leaving = jnp.any(routes[0] // per * per == bases[:, None, None], axis=1)
    before = jnp.triu(jnp.ones((rows, rows), BF16), 1)
    table = jnp.concatenate([marks.reshape(planes * per, rows), inside, leaving], axis=0)
    places = jnp.dot(table.astype(BF16), before, preferred_element_type=F32).astype(jnp.int32)
    ranks = places[: planes * per].reshape(planes, per, rows)
    at = places[planes * per : planes * per + planes]
    leave_at = places[planes * per + planes :]
    number = lax.broadcasted_iota(jnp.int32, (rows, rows), 0)
    lists = [(leaving[d][None, :] & (leave_at[d][None, :] == number)).astype(BF16) for d in range(planes)]
    turned = [x.T for x in lists]
    slot = lax.broadcasted_iota(jnp.int32, (per, capacity, rows), 1)
    weight = jnp.sum(jnp.where(hits, weights[:, :, None, :], 0.0), axis=1)
    high = lax.reduce_precision(weight, 8, 7)
    low = (weight - high).astype(BF16)
    high = high.astype(BF16)
    zero = jnp.zeros((), BF16)
    picks, mixes = [], []
    for d in range(planes):
        chosen = marks[d][:, None, :] & (ranks[d][:, None, :] == slot)
        pick = chosen.astype(BF16).reshape(per * capacity, rows)
        mix = jnp.concatenate(
            [
                jnp.where(chosen, high[d][:, None, :], zero),
                jnp.where(chosen, low[d][:, None, :], zero),
            ],
            axis=0,
        ).reshape(2 * per * capacity, rows)
        if d == 0:
            picks.append(pick)
            mixes.append(mix.T)
        else:
            listed = (inside[d][None, :] & (at[d][None, :] == number)).astype(BF16)
            across = (((1,), (1,)), ((), ()))
            picks.append(
                lax.dot_general(pick, listed, across, preferred_element_type=F32).astype(BF16)
            )
            mixes.append(
                lax.dot_general(listed, mix, across, preferred_element_type=F32).astype(BF16)
            )
    return lists[1:], turned[1:], picks, mixes


WHOLE = ()


def plane_exchange(parts, per, planes):
    if len(parts) > 1:
        return [parts[0]] + [xor_permute(parts[k], k, per * planes) for k in range(1, per)]
    groups = [[p * per + k for k in range(per)] for p in range(planes)]
    return [
        lax.all_to_all(
            parts[0], "sp", split_axis=0, concat_axis=0, axis_index_groups=groups, tiled=True
        )
    ]


def experts_relay(limit, per, planes, operands):
    hidden, normed, sent, tables, expert_gate, expert_up, expert_down = operands
    count = per * planes
    lists, turned, picks, mixes = tables
    if sent[0].shape[0] < limit:
        sent = [exact_dot(rows[:limit], normed) for rows in lists]
    came, answers, backs = [normed], [None] * planes, []
    for d in range(1, planes):
        came.append(xor_permute(sent[d - 1], d * per, count))
    for d in range(planes):
        parts = 1 if d in WHOLE else per
        slots = spread(picks[d], came[d], parts)
        arrived = plane_exchange(slots, per, planes)
        ys = run_expert(arrived, expert_gate[0], expert_up[0], expert_down[0])
        answers = plane_exchange(ys, per, planes)
        if d == 0:
            local = gather_answers(mixes[0], answers, normed.shape[0], F32)
        else:
            mixed = gather_answers(mixes[d], answers, limit, BF16)
        if d > 0:
            backs.append(xor_permute(mixed, d * per, count))
    return finish_rows(hidden, local, turned, backs)


PART = 11


def fast_shards(
    queries,
    keys,
    values,
    gate_totals,
    documents,
    stream,
    out_weight,
    norm_gain,
    routes,
    route_weights,
    expert_gate,
    expert_up,
    expert_down,
):
    if expert_gate.shape[0] != 1:
        return shards(
            queries,
            keys,
            values,
            gate_totals,
            documents,
            stream,
            out_weight,
            norm_gain,
            routes,
            route_weights,
            expert_gate,
            expert_up,
            expert_down,
        )
    count = lax.axis_size("sp")
    planes = KV_HEADS
    per = count // planes
    rows = queries.shape[0]
    index = lax.axis_index("sp")
    plane = index // per
    place = index % per
    capacity = max(2, 2 * rows * TOP // count)
    ids = jnp.stack([plane, place, per]).astype(jnp.int32)
    outs, most_all = fast_attention(
        ids, queries, keys, values, gate_totals, documents, routes, per, planes
    )
    info = jnp.concatenate([routes.T.astype(F32), route_weights.T], axis=0)
    infos = [info]
    for d in range(1, planes):
        infos.append(xor_permute(info, d * per, count))
    tables = route_tables(infos, plane, place, per, planes, capacity)
    limit = rows * PART // 16
    hidden, normed, sent = project(
        ids, outs, stream, out_weight, norm_gain, tables[0], limit, planes
    )
    operands = (hidden, normed, sent, tables, expert_gate, expert_up, expert_down)

    def usual(ops):
        return experts_relay(limit, per, planes, ops)

    def crowded(ops):
        return experts_relay(rows, per, planes, ops)

    return lax.cond(most_all <= limit, usual, crowded, operands)


def solution(mesh):
    count, tp = mesh.shape["sp"], mesh.shape["tp"]
    per = count // KV_HEADS
    fast = tp == 1 and count % KV_HEADS == 0 and per & (per - 1) == 0 and per > 1
    return jax.shard_map(
        fast_shards if fast else shards,
        mesh=mesh,
        in_specs=(
            P("sp", "tp"),
            P("sp", "tp"),
            P("sp", "tp"),
            P("sp", "tp"),
            P("sp"),
            P(("sp", "tp"), None),
            P(),
            P(),
            P(("sp", "tp"), None),
            P(("sp", "tp"), None),
            P("sp", None, "tp"),
            P("sp", None, "tp"),
            P("sp", "tp", None),
        ),
        out_specs=P(("sp", "tp"), None),
        check_vma=False,
    )
```

```python
import math

import jax
import jax.numpy as jnp
from jax import lax
from jax.experimental import pallas as pl
from jax.experimental.pallas import tpu as pltpu
from jax.sharding import PartitionSpec as P


QUERY_HEAD_COUNT = 16
KV_HEADS = 4
HD = 64
TOP = 2
GROUP = QUERY_HEAD_COUNT // KV_HEADS

EPS = 1e-06
MASKED = -1e30

EXT = 16
DOC_ROW = 3 * GROUP
COUNT_ROW = DOC_ROW + 1
ONES_ROW = DOC_ROW + 2
PACK = 2 * HD + EXT
F32 = jnp.float32
BF16 = jnp.bfloat16

CHUNK = 512
WIDE_CHUNK = 2048


def make_fold(query_rows, query_gate, key_gate_all, query_docs, first_pos, kv_local, group):
    count = query_rows.shape[0]
    scale = HD ** (-0.5)
    query_blk = query_rows.reshape(count, kv_local, group, HD)
    gate_here = query_gate.T.reshape(kv_local, group, count, 1)
    query_pos = first_pos + jnp.arange(count, dtype=jnp.int32)
    last_pos = first_pos + count - 1
    first_doc = query_docs[0]

    def block_step(carry, block_in):
        running_max, running_sum, carried = carry
        key_block, value_block, doc_block, pos_block = block_in
        width = key_block.shape[0]

        def compute(unused):
            key_heads = key_block.reshape(width, kv_local, HD)
            value_heads = value_block.reshape(width, kv_local, HD)
            gate_keys = lax.dynamic_slice_in_dim(key_gate_all, pos_block[0], width, 0).T.reshape(
                kv_local, group, 1, width
            )
            scores = (
                jnp.einsum(
                    "qkgd,nkd->kgqn", query_blk, key_heads, preferred_element_type=jnp.float32
                )
                * scale
                + gate_here
                - gate_keys
            )
            allowed = (pos_block[None, :] <= query_pos[:, None]) & (
                doc_block[None, :] == query_docs[:, None]
            )
            scores = jnp.where(allowed, scores, MASKED)
            new_max = jnp.maximum(running_max, jnp.max(scores, axis=-1))
            weights = jnp.where(allowed, jnp.exp(scores - new_max[..., None]), 0.0)
            factor = jnp.exp(running_max - new_max)
            new_sum = running_sum * factor + jnp.sum(weights, axis=-1)
            new_carried = carried * factor[..., None] + jnp.einsum(
                "kgqn,nkd->kgqd",
                weights.astype(jnp.bfloat16),
                value_heads,
                preferred_element_type=jnp.float32,
            )
            return (new_max, new_sum, new_carried)

        skipped = (pos_block[0] > last_pos) | (doc_block[width - 1] < first_doc)
        return (lax.cond(skipped, lambda unused: carry, compute, 0), None)

    def fold(carry, piece, start):
        key_piece, value_piece, doc_piece = piece
        length = key_piece.shape[0]
        width = math.gcd(length, 512)
        blocks_count = length // width
        pos_piece = jnp.arange(length, dtype=jnp.int32)
        blocks = (
            key_piece.reshape(blocks_count, width, -1),
            value_piece.reshape(blocks_count, width, -1),
            doc_piece.reshape(blocks_count, width),
            pos_piece.reshape(blocks_count, width),
        )
        carry, _ = lax.scan(block_step, carry, blocks)
        return carry

    initial = (
        jnp.full((kv_local, group, count), MASKED, jnp.float32),
        jnp.zeros((kv_local, group, count), jnp.float32),
        jnp.zeros((kv_local, group, count, HD), jnp.float32),
    )
    return (fold, initial)


def finish(running_sum, carried):
    mixed = carried / running_sum[..., None]
    count = mixed.shape[2]
    return jnp.transpose(mixed, (2, 0, 1, 3)).reshape(count, -1).astype(jnp.bfloat16)


def shards(
    queries,
    keys,
    values,
    gate_totals,
    documents,
    stream,
    out_weight,
    norm_gain,
    routes,
    route_weights,
    expert_gate,
    expert_up,
    expert_down,
):
    tp_count = lax.axis_size("tp")
    tp_index = lax.axis_index("tp")
    sp_index = lax.axis_index("sp")
    group = QUERY_HEAD_COUNT // KV_HEADS
    tok_local = queries.shape[0]
    own_rows = tok_local // tp_count
    first_row = sp_index * tok_local
    query_rows = lax.all_to_all(queries, "tp", split_axis=0, concat_axis=1, tiled=True)
    key_whole, value_whole = (
        lax.all_gather(keys, "tp", axis=1, tiled=True),
        lax.all_gather(values, "tp", axis=1, tiled=True),
    )
    gate_whole = lax.all_gather(gate_totals, "tp", axis=1, tiled=True)
    key_gate_all = lax.all_gather(gate_whole, "sp", axis=0, tiled=True)
    query_gate = lax.dynamic_slice_in_dim(gate_whole, tp_index * own_rows, own_rows, 0)
    query_docs = lax.dynamic_slice_in_dim(documents, tp_index * own_rows, own_rows, 0)
    fold, initial = make_fold(
        query_rows,
        query_gate,
        key_gate_all,
        query_docs,
        first_row + tp_index * own_rows,
        KV_HEADS,
        group,
    )
    _, running_sum, carried = fold(
        initial,
        (
            lax.all_gather(key_whole, "sp", axis=0, tiled=True),
            lax.all_gather(value_whole, "sp", axis=0, tiled=True),
            lax.all_gather(documents, "sp", axis=0, tiled=True),
        ),
        jnp.int32(0),
    )
    attended = finish(running_sum, carried)
    hidden = (
        stream.astype(jnp.float32)
        + jnp.dot(attended, out_weight, preferred_element_type=jnp.float32)
    ).astype(jnp.bfloat16)
    hidden_f = hidden.astype(jnp.float32)
    normed = (
        hidden_f
        * lax.rsqrt(jnp.mean(hidden_f * hidden_f, axis=-1, keepdims=True) + EPS)
        * norm_gain
    ).astype(jnp.bfloat16)
    return experts_direct(
        hidden, normed, routes, route_weights, expert_gate, expert_up, expert_down
    )


def experts_direct(hidden, normed, routes, route_weights, expert_gate, expert_up, expert_down):
    tp_count = lax.axis_size("tp")
    sp_count = lax.axis_size("sp")
    hidden_f = hidden.astype(jnp.float32)
    own_rows = hidden.shape[0]
    tok_local = own_rows * tp_count
    local_experts = expert_gate.shape[0]
    experts_total = local_experts * sp_count
    capacity = max(2, 2 * tok_local * TOP // (tp_count * experts_total))
    flat = routes.reshape(-1)
    hits = (flat[:, None] == jnp.arange(experts_total, dtype=jnp.int32)[None, :]).astype(jnp.int32)
    slot_index = jnp.sum(jnp.cumsum(hits, axis=0) * hits, axis=1) - 1
    target = flat * capacity + slot_index
    entry_rows = jnp.repeat(normed, TOP, axis=0)
    outgoing = (
        jnp.zeros((experts_total * capacity, normed.shape[1]), jnp.bfloat16)
        .at[target]
        .set(entry_rows)
    )
    outgoing = outgoing.reshape(experts_total, capacity, -1)
    arrived = lax.all_to_all(outgoing, "sp", split_axis=0, concat_axis=0, tiled=True)
    slots = arrived.shape[1]
    both_halves = lax.all_gather(arrived, "tp", axis=0, tiled=True)
    grouped = both_halves.reshape(tp_count * sp_count, local_experts, slots, -1)
    gate = jnp.einsum("secd,edf->secf", grouped, expert_gate, preferred_element_type=jnp.float32)
    upper = jnp.einsum("secd,edf->secf", grouped, expert_up, preferred_element_type=jnp.float32)
    inner = (jax.nn.silu(gate) * upper).astype(jnp.bfloat16)
    partial_value = jnp.einsum(
        "secf,efd->secd", inner, expert_down, preferred_element_type=jnp.float32
    )
    partial_value = lax.optimization_barrier(partial_value.astype(jnp.bfloat16)).astype(jnp.float32)
    summed = lax.psum_scatter(
        partial_value.reshape(tp_count * sp_count * local_experts, slots, -1).astype(jnp.bfloat16),
        "tp",
        scatter_dimension=0,
        tiled=True,
    )
    returned = lax.all_to_all(summed, "sp", split_axis=0, concat_axis=0, tiled=True)
    answers = returned.reshape(experts_total * capacity, -1)[target].reshape(own_rows, TOP, -1)
    routed = jnp.sum(route_weights[..., None] * answers.astype(jnp.float32), axis=1)
    return (hidden_f + routed).astype(jnp.bfloat16)


def xor_permute(x, distance, count):
    return lax.ppermute(x, "sp", [(s, s ^ distance) for s in range(count)])


def attention_kernel(per, planes, blk, dists, *refs):
    nq = len(dists)
    ids_ref = refs[0]
    q_refs = refs[1 : 1 + nq]
    kv_refs = refs[1 + nq : 1 + nq + per]
    o_refs = refs[1 + nq + per : 1 + 2 * nq + per]
    most_ref = refs[1 + 2 * nq + per]
    kvs, qa, m_ref, acc_ref, o_all, sems = refs[2 + 2 * nq + per :]
    copies = [
        pltpu.make_async_copy(kv_refs[k], kvs.at[pl.ds(k * planes, planes)], sems.at[k])
        for k in range(per)
    ]
    for c in copies:
        c.start()
    plane, place = ids_ref[0], ids_ref[1]
    lane = lax.broadcasted_iota(jnp.int32, (blk, EXT), 1)
    for i in range(nq):
        for h in range(GROUP):
            qa[i * GROUP + h, :, 0:HD] = q_refs[i][:, h * HD : (h + 1) * HD] * jnp.asarray(
                HD ** (-0.5), BF16
            )
            pick = (lane == h) | (lane == GROUP + h) | (lane == 2 * GROUP + h)
            qa[i * GROUP + h, :, HD : HD + EXT] = jnp.where(pick, -1.0, 0.0).astype(BF16)
    for c in copies:
        c.wait()
    ext_sum = jnp.zeros((EXT, blk), F32)
    ext_max = jnp.zeros((EXT, blk), F32)
    for b in range(per * planes):
        ext = kvs[b, HD : HD + EXT, :].astype(F32)
        ext_sum = ext_sum + ext
        ext_max = jnp.maximum(ext_max, ext)
    row = lax.broadcasted_iota(jnp.int32, (EXT, blk), 0)
    later = jnp.sum(jnp.where(row == DOC_ROW, ext_sum, 0.0)).astype(jnp.int32)
    border = per * planes * blk - later
    most_ref[0] = jnp.max(jnp.where(row == COUNT_ROW, ext_max, 0.0)).astype(jnp.int32)

    def one_block(i, unused):
        dist = jnp.int32(dists[0])
        for n in range(1, nq):
            dist = jnp.where(i == n, dists[n], dist)
        block = (plane ^ dist) * per + place
        first = block * blk
        begin = jnp.where(first >= border, border, 0)
        last_begin = jnp.where(first + blk > border, border, 0)
        low = begin // blk
        free = jnp.minimum(block, (last_begin + blk - 1) // blk)
        free = free + lax.rem(block - free, 2)
        for h in range(GROUP):
            m_ref[h] = jnp.full((blk, 128), MASKED, F32)
            acc_ref[h] = jnp.zeros((blk, EXT + HD), F32)

        def where_is(kb):
            return ((kb % per) ^ place) * planes + ((kb // per) ^ plane)

        def step(kbs, masked):
            at = [where_is(kb) for kb in kbs]
            if masked:
                pos_q = first + lax.broadcasted_iota(jnp.int32, (blk, blk), 0)
                pos_k = kbs[0] * blk + lax.broadcasted_iota(jnp.int32, (blk, blk), 1)
                start_q = jnp.where(pos_q >= border, border, 0)
                allowed = (pos_k <= pos_q) & (pos_k >= start_q)
            for h in range(GROUP):
                scores = [
                    jnp.dot(
                        qa[i * GROUP + h], kvs[a, 0 : HD + EXT, :], preferred_element_type=F32
                    )
                    for a in at
                ]
                if masked:
                    scores = [jnp.where(allowed, s, MASKED) for s in scores]
                old = m_ref[h]
                top = scores[0]
                for s in scores[1:]:
                    top = jnp.maximum(top, s)
                new = jnp.maximum(old, jnp.max(top, axis=1, keepdims=True))
                wide = jnp.concatenate([new] * (blk // 128), axis=1)
                mixed = acc_ref[h] * jnp.exp(old - new)[:, 0 : EXT + HD]
                for s, a in zip(scores, at):
                    weights = jnp.exp(s - wide)
                    if masked:
                        weights = jnp.where(allowed, weights, 0.0)
                    mixed = mixed + lax.dot_general(
                        weights.astype(BF16),
                        kvs[a, HD:PACK, :],
                        (((1,), (1,)), ((), ())),
                        preferred_element_type=F32,
                    )
                m_ref[h] = new
                acc_ref[h] = mixed

        count = free - low + 1

        def masked_step(n, unused):
            step([jnp.where(n == count - 1, block, low + n)], True)
            return 0

        def free_step(n, unused):
            step([free + 2 * n, free + 2 * n + 1], False)
            return 0

        lax.fori_loop(0, (block - free) // 2, free_step, 0)
        lax.fori_loop(0, count, masked_step, 0)
        for h in range(GROUP):
            mixed = acc_ref[h]
            o_all[i, :, h * HD : (h + 1) * HD] = (
                mixed[:, EXT : EXT + HD] / mixed[:, ONES_ROW : ONES_ROW + 1]
            ).astype(BF16)
        return 0

    lax.fori_loop(0, nq, one_block, 0)
    for i in range(nq):
        o_refs[i][...] = o_all[i]


def run_attention(ids, q_blocks, packs, dists, per, planes):
    blk = q_blocks[0].shape[0]
    nq = len(dists)
    vm = pl.BlockSpec(memory_space=pltpu.VMEM)
    sm = pl.BlockSpec(memory_space=pltpu.SMEM)
    hb = pl.BlockSpec(memory_space=pl.ANY)
    pairs = nq * GROUP * blk * per * planes * blk
    out = pl.pallas_call(
        lambda *refs: attention_kernel(per, planes, blk, dists, *refs),
        out_shape=[jax.ShapeDtypeStruct((blk, GROUP * HD), BF16)] * nq
        + [jax.ShapeDtypeStruct((1,), jnp.int32)],
        in_specs=[sm] + [vm] * nq + [hb] * per,
        out_specs=[vm] * nq + [sm],
        scratch_shapes=[
            pltpu.VMEM((per * planes, PACK, blk), BF16),
            pltpu.VMEM((nq * GROUP, blk, HD + EXT), BF16),
            pltpu.VMEM((GROUP, blk, 128), F32),
            pltpu.VMEM((GROUP, blk, EXT + HD), F32),
            pltpu.VMEM((nq, blk, GROUP * HD), BF16),
            pltpu.SemaphoreType.DMA((per,)),
        ],
        compiler_params=pltpu.CompilerParams(vmem_limit_bytes=48 * 1024 * 1024),
        cost_estimate=pl.CostEstimate(
            flops=pairs * 300, transcendentals=pairs, bytes_accessed=4 << 20
        ),
        name="attention",
    )(ids, *q_blocks, *packs)
    return out[:nq], out[nq]


def vmem_spec():
    return pl.BlockSpec(memory_space=pltpu.VMEM)


def prepare_kernel(planes, *refs):
    ids_ref, key_ref, value_ref, gate_ref, doc_ref, route_ref, query_ref = refs[:7]
    pack_refs, q_refs, packed = refs[7 : 7 + planes], refs[7 + planes : 7 + 2 * planes], refs[-1]
    plane, per = ids_ref[0], ids_ref[2]
    heads, blk = gate_ref.shape
    rest = gate_ref[...]
    pieces = []
    for _ in range(3):
        piece = rest.astype(BF16)
        pieces.append(piece)
        rest = rest - piece.astype(F32)
    goes = route_ref[...] // per
    most = jnp.zeros((1, 1), F32)
    for p in range(planes):
        there = jnp.max((goes == p).astype(F32), axis=0, keepdims=True)
        most = jnp.maximum(most, jnp.sum(there, axis=1, keepdims=True))
    row = lax.broadcasted_iota(jnp.int32, (EXT, blk), 0)
    fixed = jnp.where(row == DOC_ROW, doc_ref[...].astype(F32), 0.0)
    fixed = fixed + jnp.where(row == COUNT_ROW, most, 0.0) + jnp.where(row == ONES_ROW, 1.0, 0.0)
    to = lax.broadcasted_iota(jnp.int32, (EXT, heads), 0)
    source = lax.broadcasted_iota(jnp.int32, (EXT, heads), 1)
    key_turned = key_ref[...].astype(F32).T.astype(BF16)
    value_turned = value_ref[...].astype(F32).T.astype(BF16)
    for g in range(KV_HEADS):
        extra = fixed
        for part, piece in enumerate(pieces):
            at = to - part * GROUP
            pick = (at >= 0) & (at < GROUP) & (source == g * GROUP + at)
            extra = extra + jnp.dot(
                jnp.where(pick, 1.0, 0.0).astype(BF16), piece, preferred_element_type=F32
            )
        packed[g, 0:HD, :] = key_turned[g * HD : (g + 1) * HD]
        packed[g, HD : HD + EXT, :] = extra.astype(BF16)
        packed[g, HD + EXT : PACK, :] = value_turned[g * HD : (g + 1) * HD]
    size = GROUP * HD
    for d in range(planes):
        pack_refs[d][0] = packed[plane ^ d]
        q_refs[d][...] = query_ref[:, pl.ds(pl.multiple_of((plane ^ d) * size, size), size)]


def prepare(ids, keys, values, gates, documents, routes, queries, planes):
    blk = queries.shape[0]
    sm = pl.BlockSpec(memory_space=pltpu.SMEM)
    out = pl.pallas_call(
        lambda *refs: prepare_kernel(planes, *refs),
        out_shape=[jax.ShapeDtypeStruct((1, PACK, blk), BF16)] * planes
        + [jax.ShapeDtypeStruct((blk, GROUP * HD), BF16)] * planes,
        in_specs=[sm] + [vmem_spec()] * 6,
        out_specs=[vmem_spec()] * (2 * planes),
        scratch_shapes=[pltpu.VMEM((KV_HEADS, PACK, blk), BF16)],
        name="prepare",
    )(ids, keys, values, gates.T, documents.reshape(1, blk), routes.T, queries)
    return out[:planes], out[planes:]


def fast_attention(ids, queries, keys, values, gate_totals, documents, routes, per, planes):
    count = per * planes
    own, q_groups = prepare(
        ids, keys, values, gate_totals, documents, routes, queries, planes
    )
    column, q_blocks = [own[0]], [q_groups[0]]
    for d in range(1, planes):
        column.append(xor_permute(own[d], d * per, count))
        q_blocks.append(xor_permute(q_groups[d], d * per, count))
    column = jnp.concatenate(column, axis=0)
    packs = {0: column}
    for k in range(2, per, 2):
        packs[k] = xor_permute(column, k, count)
    for k in range(0, per, 2):
        packs[k + 1] = xor_permute(packs[k], 1, count)
    packs = [packs[k] for k in range(per)]
    outs = [None] * planes
    far = list(range(planes - 1, 0, -1))
    far_out, most_all = run_attention(ids, [q_blocks[d] for d in far], packs, far, per, planes)
    for d, o in zip(far, far_out):
        outs[d] = xor_permute(o, d * per, count)
    near_out, _ = run_attention(ids, [q_blocks[0]], packs, [0], per, planes)
    outs[0] = near_out[0]
    return outs, most_all[0]


def project_kernel(planes, limit, *refs):
    ids_ref, stream_ref, weight_ref, gain_ref = refs[:4]
    o_refs = refs[4 : 4 + planes]
    list_refs = refs[4 + planes : 3 + 2 * planes]
    hidden_ref, normed_ref = refs[3 + 2 * planes : 5 + 2 * planes]
    sent_refs = refs[5 + 2 * planes :]
    plane = ids_ref[0]
    rows = o_refs[0].shape[1]
    blk, width = stream_ref.shape
    attended = [o[...] for o in o_refs]

    def columns(c, squares):
        at = pl.ds(pl.multiple_of(c * WIDE_CHUNK, WIDE_CHUNK), WIDE_CHUNK)
        total = stream_ref[:, at].astype(F32)
        for d in range(planes):
            weight = weight_ref[pl.ds(pl.multiple_of((plane ^ d) * rows, rows), rows), at]
            total = total + jnp.dot(attended[d], weight, preferred_element_type=F32)
        hidden = total.astype(BF16)
        hidden_ref[:, at] = hidden
        hidden_f = hidden.astype(F32)
        return squares + jnp.sum(hidden_f * hidden_f, axis=-1, keepdims=True)

    squares = lax.fori_loop(0, width // WIDE_CHUNK, columns, jnp.zeros((blk, 1), F32))
    scale = lax.rsqrt(squares / width + EPS)

    def send(c, unused):
        at = pl.ds(pl.multiple_of(c * WIDE_CHUNK, WIDE_CHUNK), WIDE_CHUNK)
        normed = (hidden_ref[:, at].astype(F32) * scale * gain_ref[:, at]).astype(BF16)
        normed_ref[:, at] = normed
        for d in range(1, planes):
            sent_refs[d - 1][:, at] = jnp.dot(
                list_refs[d - 1][0:limit, :], normed, preferred_element_type=F32
            ).astype(BF16)
        return 0

    lax.fori_loop(0, width // WIDE_CHUNK, send, 0)


def project(ids, outs, stream, out_weight, norm_gain, lists, limit, planes):
    rows, width = stream.shape
    flops = 2 * rows * width * (out_weight.shape[0] + 3 * limit)
    result = pl.pallas_call(
        lambda *refs: project_kernel(planes, limit, *refs),
        out_shape=[jax.ShapeDtypeStruct((rows, width), BF16)] * 2
        + [jax.ShapeDtypeStruct((limit, width), BF16)] * (planes - 1),
        in_specs=[pl.BlockSpec(memory_space=pltpu.SMEM)] + [vmem_spec()] * (2 + 2 * planes),
        out_specs=[vmem_spec()] * (1 + planes),
        compiler_params=pltpu.CompilerParams(vmem_limit_bytes=40 * 1024 * 1024),
        cost_estimate=pl.CostEstimate(flops=flops, transcendentals=0, bytes_accessed=8 << 20),
        name="project",
    )(ids, stream, out_weight, norm_gain.reshape(1, width), *outs, *lists)
    return result[0], result[1], result[2:]


def exact_dot(a, b):
    return jnp.dot(a, b, preferred_element_type=F32).astype(BF16)


def spread_kernel(pick_ref, rows_ref, *outs):
    pick = pick_ref[:, 0 : rows_ref.shape[0]]
    size = outs[0].shape[0]

    def columns(c, unused):
        at = pl.ds(pl.multiple_of(c * CHUNK, CHUNK), CHUNK)
        slots = jnp.dot(pick, rows_ref[:, at], preferred_element_type=F32).astype(BF16)
        for k, out in enumerate(outs):
            out[:, at] = slots[k * size : (k + 1) * size]
        return 0

    lax.fori_loop(0, rows_ref.shape[1] // CHUNK, columns, 0)


def spread(pick, rows, per):
    slots = pick.shape[0]
    limit, width = rows.shape
    return pl.pallas_call(
        spread_kernel,
        out_shape=[jax.ShapeDtypeStruct((slots // per, width), BF16)] * per,
        in_specs=[vmem_spec()] * 2,
        out_specs=[vmem_spec()] * per,
        cost_estimate=pl.CostEstimate(
            flops=2 * slots * limit * width, transcendentals=0, bytes_accessed=2 << 20
        ),
        name="spread",
    )(pick, rows)


def expert_kernel(per, *refs):
    x_refs = refs[:per]
    gate_ref, up_ref, down_ref = refs[per : per + 3]
    o_refs = refs[per + 3 : 2 * per + 3]
    x_all, acc = refs[2 * per + 3 :]
    step = pl.program_id(0)
    size = x_refs[0].shape[0]

    @pl.when(step == 0)
    def fill():
        for k in range(per):
            x_all[k * size : (k + 1) * size, :] = x_refs[k][...]
        acc[...] = jnp.zeros(acc.shape, F32)

    x = x_all[...]
    gate = jnp.dot(x, gate_ref[...], preferred_element_type=F32)
    upper = jnp.dot(x, up_ref[...], preferred_element_type=F32)
    inner = (gate * jax.nn.sigmoid(gate) * upper).astype(BF16)
    acc[...] = acc[...] + jnp.dot(inner, down_ref[...], preferred_element_type=F32)

    @pl.when(step == pl.num_programs(0) - 1)
    def last():
        for k in range(per):
            o_refs[k][...] = acc[k * size : (k + 1) * size, :].astype(BF16)


def run_expert(xs, expert_gate, expert_up, expert_down):
    per = len(xs)
    size, width = xs[0].shape
    units = expert_gate.shape[1]
    chunk = min(256, units)
    whole = pl.BlockSpec((size, width), lambda f: (0, 0))
    return pl.pallas_call(
        lambda *refs: expert_kernel(per, *refs),
        grid=(units // chunk,),
        out_shape=[jax.ShapeDtypeStruct((size, width), BF16)] * per,
        in_specs=[whole] * per
        + [
            pl.BlockSpec((width, chunk), lambda f: (0, f)),
            pl.BlockSpec((width, chunk), lambda f: (0, f)),
            pl.BlockSpec((chunk, width), lambda f: (f, 0)),
        ],
        out_specs=[whole] * per,
        scratch_shapes=[
            pltpu.VMEM((per * size, width), BF16),
            pltpu.VMEM((per * size, width), F32),
        ],
        compiler_params=pltpu.CompilerParams(
            dimension_semantics=("arbitrary",), vmem_limit_bytes=40 * 1024 * 1024
        ),
        cost_estimate=pl.CostEstimate(
            flops=6 * per * size * width * units,
            transcendentals=per * size * units,
            bytes_accessed=14 << 20,
        ),
        name="expert",
    )(*xs, expert_gate, expert_up, expert_down)


def gather_kernel(limit, *refs):
    mix_ref, out_ref = refs[0], refs[-1]

    def columns(c, unused):
        at = pl.ds(pl.multiple_of(c * CHUNK, CHUNK), CHUNK)
        answers = jnp.concatenate([r[:, at] for r in refs[1:-1]], axis=0)
        slots = answers.shape[0]
        total = jnp.dot(mix_ref[0:limit, 0:slots], answers, preferred_element_type=F32)
        total = total + jnp.dot(mix_ref[0:limit, slots:], answers, preferred_element_type=F32)
        out_ref[:, at] = total.astype(out_ref.dtype)
        return 0

    lax.fori_loop(0, out_ref.shape[1] // CHUNK, columns, 0)


def gather_answers(mix, answers, limit, dtype):
    width = answers[0].shape[1]
    return pl.pallas_call(
        lambda *refs: gather_kernel(limit, *refs),
        out_shape=jax.ShapeDtypeStruct((limit, width), dtype),
        in_specs=[vmem_spec()] * (1 + len(answers)),
        out_specs=vmem_spec(),
        cost_estimate=pl.CostEstimate(
            flops=2 * limit * mix.shape[1] * width, transcendentals=0, bytes_accessed=2 << 20
        ),
        name="gather",
    )(mix, *answers)


def finish_kernel(limit, *refs):
    hidden_ref, local_ref, out_ref = refs[0], refs[1], refs[-1]
    others = (len(refs) - 3) // 2
    total = hidden_ref[...].astype(F32) + local_ref[...]
    for turned, back in zip(refs[2 : 2 + others], refs[2 + others : 2 + 2 * others]):
        total = total + jnp.dot(
            turned[:, 0:limit], back[...], preferred_element_type=F32
        )
    out_ref[...] = total.astype(BF16)


def finish_rows(hidden, local, turned, backs):
    rows, width = hidden.shape
    limit = backs[0].shape[0]
    chunk = min(512, width)
    columns = lambda size: pl.BlockSpec((size, chunk), lambda f: (0, f))
    return pl.pallas_call(
        lambda *refs: finish_kernel(limit, *refs),
        grid=(width // chunk,),
        out_shape=jax.ShapeDtypeStruct((rows, width), BF16),
        in_specs=[columns(rows)] * 2
        + [pl.BlockSpec((rows, rows), lambda f: (0, 0))] * len(turned)
        + [columns(limit)] * len(backs),
        out_specs=columns(rows),
        compiler_params=pltpu.CompilerParams(dimension_semantics=("arbitrary",)),
        name="finish",
    )(hidden, local, *turned, *backs)


def route_tables(infos, plane, place, per, planes, capacity):
    rows = infos[0].shape[1]
    routes = jnp.stack([info[:TOP] for info in infos]).astype(jnp.int32)
    weights = jnp.stack([info[TOP:] for info in infos])
    spots = jnp.arange(per, dtype=jnp.int32)
    ids = plane * per + jnp.stack([spots if d in WHOLE else place ^ spots for d in range(planes)])
    hits = routes[:, :, None, :] == ids[:, None, :, None]
    marks = jnp.any(hits, axis=1)
    inside = jnp.any(marks, axis=1)
    bases = (plane ^ jnp.arange(planes, dtype=jnp.int32)) * per
    leaving = jnp.any(routes[0] // per * per == bases[:, None, None], axis=1)
    before = jnp.triu(jnp.ones((rows, rows), BF16), 1)
    table = jnp.concatenate([marks.reshape(planes * per, rows), inside, leaving], axis=0)
    places = jnp.dot(table.astype(BF16), before, preferred_element_type=F32).astype(jnp.int32)
    ranks = places[: planes * per].reshape(planes, per, rows)
    at = places[planes * per : planes * per + planes]
    leave_at = places[planes * per + planes :]
    number = lax.broadcasted_iota(jnp.int32, (rows, rows), 0)
    lists = [(leaving[d][None, :] & (leave_at[d][None, :] == number)).astype(BF16) for d in range(planes)]
    turned = [x.T for x in lists]
    slot = lax.broadcasted_iota(jnp.int32, (per, capacity, rows), 1)
    weight = jnp.sum(jnp.where(hits, weights[:, :, None, :], 0.0), axis=1)
    high = lax.reduce_precision(weight, 8, 7)
    low = (weight - high).astype(BF16)
    high = high.astype(BF16)
    zero = jnp.zeros((), BF16)
    picks, mixes = [], []
    for d in range(planes):
        chosen = marks[d][:, None, :] & (ranks[d][:, None, :] == slot)
        pick = chosen.astype(BF16).reshape(per * capacity, rows)
        mix = jnp.concatenate(
            [
                jnp.where(chosen, high[d][:, None, :], zero),
                jnp.where(chosen, low[d][:, None, :], zero),
            ],
            axis=0,
        ).reshape(2 * per * capacity, rows)
        if d == 0:
            picks.append(pick)
            mixes.append(mix.T)
        else:
            listed = (inside[d][None, :] & (at[d][None, :] == number)).astype(BF16)
            across = (((1,), (1,)), ((), ()))
            picks.append(
                lax.dot_general(pick, listed, across, preferred_element_type=F32).astype(BF16)
            )
            mixes.append(
                lax.dot_general(listed, mix, across, preferred_element_type=F32).astype(BF16)
            )
    return lists[1:], turned[1:], picks, mixes


WHOLE = ()


def plane_exchange(parts, per, planes):
    if len(parts) > 1:
        return [parts[0]] + [xor_permute(parts[k], k, per * planes) for k in range(1, per)]
    groups = [[p * per + k for k in range(per)] for p in range(planes)]
    return [
        lax.all_to_all(
            parts[0], "sp", split_axis=0, concat_axis=0, axis_index_groups=groups, tiled=True
        )
    ]


def experts_relay(limit, per, planes, operands):
    hidden, normed, sent, tables, expert_gate, expert_up, expert_down = operands
    count = per * planes
    _, turned, picks, mixes = tables
    came, answers, backs = [normed], [None] * planes, []
    for d in range(1, planes):
        came.append(xor_permute(sent[d - 1], d * per, count))
    for d in range(planes):
        parts = 1 if d in WHOLE else per
        slots = spread(picks[d], came[d], parts)
        arrived = plane_exchange(slots, per, planes)
        ys = run_expert(arrived, expert_gate[0], expert_up[0], expert_down[0])
        answers = plane_exchange(ys, per, planes)
        if d == 0:
            local = gather_answers(mixes[0], answers, normed.shape[0], F32)
        else:
            mixed = gather_answers(mixes[d], answers, limit, BF16)
        if d > 0:
            backs.append(xor_permute(mixed, d * per, count))
    return finish_rows(hidden, local, turned, backs)


def experts_looped(per, planes, operands):
    hidden, normed, _, tables, expert_gate, expert_up, expert_down = operands
    count = per * planes
    rows = normed.shape[0]
    lists, turned, picks, mixes = tables
    came = [normed]
    for d in range(1, planes):
        came.append(xor_permute(exact_dot(lists[d - 1], normed), d * per, count))
    came, picks, mixes = jnp.stack(came), jnp.stack(picks), jnp.stack(mixes)

    def one_plane(d, done):
        slots = spread(picks[d], came[d], per)
        arrived = plane_exchange(slots, per, planes)
        ys = run_expert(arrived, expert_gate[0], expert_up[0], expert_down[0])
        answers = plane_exchange(ys, per, planes)
        mixed = gather_answers(mixes[d], answers, rows, BF16)
        return lax.dynamic_update_index_in_dim(done, mixed, d, 0)

    done = lax.fori_loop(0, planes, one_plane, jnp.zeros_like(came))
    backs = [xor_permute(done[d], d * per, count) for d in range(1, planes)]
    return finish_rows(hidden, done[0].astype(F32), turned, backs)


PART = 11


def fast_shards(
    queries,
    keys,
    values,
    gate_totals,
    documents,
    stream,
    out_weight,
    norm_gain,
    routes,
    route_weights,
    expert_gate,
    expert_up,
    expert_down,
):
    if expert_gate.shape[0] != 1:
        return shards(
            queries,
            keys,
            values,
            gate_totals,
            documents,
            stream,
            out_weight,
            norm_gain,
            routes,
            route_weights,
            expert_gate,
            expert_up,
            expert_down,
        )
    count = lax.axis_size("sp")
    planes = KV_HEADS
    per = count // planes
    rows = queries.shape[0]
    index = lax.axis_index("sp")
    plane = index // per
    place = index % per
    capacity = max(2, 2 * rows * TOP // count)
    ids = jnp.stack([plane, place, per]).astype(jnp.int32)
    outs, most_all = fast_attention(
        ids, queries, keys, values, gate_totals, documents, routes, per, planes
    )
    info = jnp.concatenate([routes.T.astype(F32), route_weights.T], axis=0)
    infos = [info]
    for d in range(1, planes):
        infos.append(xor_permute(info, d * per, count))
    tables = route_tables(infos, plane, place, per, planes, capacity)
    limit = rows * PART // 16
    hidden, normed, sent = project(
        ids, outs, stream, out_weight, norm_gain, tables[0], limit, planes
    )
    operands = (hidden, normed, sent, tables, expert_gate, expert_up, expert_down)

    def usual(ops):
        return experts_relay(limit, per, planes, ops)

    def crowded(ops):
        return experts_looped(per, planes, ops)

    return lax.cond(most_all <= limit, usual, crowded, operands)


def solution(mesh):
    count, tp = mesh.shape["sp"], mesh.shape["tp"]
    per = count // KV_HEADS
    fast = tp == 1 and count % KV_HEADS == 0 and per & (per - 1) == 0 and per > 1
    return jax.shard_map(
        fast_shards if fast else shards,
        mesh=mesh,
        in_specs=(
            P("sp", "tp"),
            P("sp", "tp"),
            P("sp", "tp"),
            P("sp", "tp"),
            P("sp"),
            P(("sp", "tp"), None),
            P(),
            P(),
            P(("sp", "tp"), None),
            P(("sp", "tp"), None),
            P("sp", None, "tp"),
            P("sp", None, "tp"),
            P("sp", "tp", None),
        ),
        out_specs=P(("sp", "tp"), None),
        check_vma=False,
    )
```
